32 devices in a mesh: sp: 4 (over y, core), dp: 8 (over z, x).
Axes of the slice: x: 2, y: 2, z: 4, core: 2. Of those that a mesh axis runs over, the one named last changes fastest.
Arguments:
- queries: bfloat16 [8, 704, 2048], P('dp', 'sp'), may hold values from -24 to 24, as said below
- keys: bfloat16 [8, 704, 256], P('dp', 'sp'), may hold values from -24 to 24, as said below
- tokens: bfloat16 [8, 704, 2304], P('dp', 'sp'), may hold values from -18 to 18
- w_value: bfloat16 [2304, 256], P('dp'), may hold values from -0.125 to 0.125
- q_gain: float32 [128], replicated, may hold values from 0.5 to 6, as said below
- k_gain: float32 [128], replicated, may hold values from 0.5 to 6, as said below
Outputs:
- attended: bfloat16 [8, 704, 2048], P('dp', 'sp')
The draws below stay inside these ranges and needn't reach their ends.
Inputs may be any that keep to these rules, and one draw needn't show every extreme that they name: `queries`: real-valued projected query entries. `keys`: real-valued projected key entries. `q_gain`: positive gains. `k_gain`: positive gains.
All inputs are finite; a program needn't handle non-finite values.
Results may differ from the reference program's by a relative error of at most 0.0022.
The reference program's roundings to bfloat16 on the way (of `values`, `query_rot`, `key_rot` and `probability`) count: a program that leaves them out, or rounds other values in their place, can miss the bound.
Values may be sent and summed in bfloat16 or wider, within the bound.
A program may use at most 64 MiB of HBM per device.

```python
import math
import jax
import jax.numpy as jnp
from jax import lax

D = 2304
HD = 128
QH = 16
KVH = 2
GRID_W = 64
LEN = 704
BATCH = 8


def shared_pair(key):
    key_draw = jnp.clip(jax.random.normal(jax.random.fold_in(key, 11), (BATCH, LEN, KVH * HD), jnp.float32), -6.0, 6.0)
    query_draw = jnp.clip(jax.random.normal(jax.random.fold_in(key, 12), (BATCH, LEN, QH * HD), jnp.float32), -6.0, 6.0)
    return (query_draw, key_draw)


def draw_queries(key, part):
    return shared_pair(key)[0].astype(jnp.bfloat16)


def draw_keys(key, part):
    return shared_pair(key)[1].astype(jnp.bfloat16)


def gain_draw(key):
    return jnp.exp(jax.random.uniform(key, (HD,), jnp.float32, jnp.log(0.6), jnp.log(1.8)))


def draw_q_gain(key, part):
    return gain_draw(jax.random.fold_in(key, 21))


def draw_k_gain(key, part):
    return gain_draw(jax.random.fold_in(key, 22))


def levels(stream_key, dims, shards, smallest, top_value):
    def one(dim, parts):
        heights = jax.random.uniform(jax.random.fold_in(jax.random.fold_in(stream_key, 6), dim), (parts,), jnp.float32, smallest / len(shards), top_value / len(shards))
        return jnp.repeat(jnp.exp(heights), dims[dim] // parts).reshape((-1,) + (1,) * (len(dims) - dim - 1))

    level = one(*shards[0])
    for cut in shards[1:]:
        level = level * one(*cut)
    return level


def normal_values(stream_key, shape, width, most, shards=(), kind=jnp.bfloat16):
    array = jax.random.normal(stream_key, shape, jnp.float32) * width
    if len(shards) > 0:
        array = levels(stream_key, shape, shards, -0.22, 0.18) * array
    return jnp.clip(array, min=-most, max=most).astype(kind)


def setup_inputs(seed: int = 0) -> dict:
    key_list = jax.random.split(jax.random.key(seed), 7)
    queries = draw_queries(jax.random.fold_in(key_list[6], 71), 0)
    keys = draw_keys(jax.random.fold_in(key_list[6], 71), 0)
    tokens = normal_values(key_list[2], (BATCH, LEN, D), 3.0, 18.0, ((0, 8), (1, 4)))
    w_value = normal_values(key_list[3], (D, KVH * HD), D ** -0.5, 0.125, ((0, 8),))
    q_gain = draw_q_gain(jax.random.fold_in(key_list[6], 71), 0)
    k_gain = draw_k_gain(jax.random.fold_in(key_list[6], 71), 0)
    return {"queries": queries, "keys": keys, "tokens": tokens, "w_value": w_value, "q_gain": q_gain, "k_gain": k_gain}


epsilon = 1e-06

def unit_rms(vectors, scaling):
    return vectors * lax.rsqrt(lax.optimization_barrier(jnp.mean(vectors * vectors, axis=-1, keepdims=True)) + epsilon) * scaling

def rotary(vectors, row_pos, col_pos):
    head_width = vectors.shape[-1]
    half_width = head_width // 2
    quarter = half_width // 2
    frequency = 10000.0 ** (-jnp.arange(quarter, dtype=jnp.float32) * 2.0 / half_width)

    def rotate_half(section, angle_pos):
        angles = angle_pos[:, None, None] * frequency
        cosine = jnp.cos(angles)
        sine_table = jnp.sin(angles)
        leading = section[..., :quarter]
        second = section[..., quarter:]
        return jnp.concatenate([leading * cosine - second * sine_table, second * cosine + leading * sine_table], axis=-1)
    return jnp.concatenate([rotate_half(vectors[..., :half_width], row_pos), rotate_half(vectors[..., half_width:], col_pos)], axis=-1)

def reference(queries, keys, tokens, w_value, q_gain, k_gain):
    group = QH // KVH
    positions = jnp.arange(LEN, dtype=jnp.int32)
    row_pos = (positions // GRID_W).astype(jnp.float32)
    col_pos = (positions % GRID_W).astype(jnp.float32)
    block_rows = math.gcd(LEN, 512)

    def one_sequence(inputs):
        query_rows, key_rows, token_rows = inputs
        values = jnp.dot(token_rows, w_value, preferred_element_type=jnp.float32)
        values = lax.optimization_barrier(values.astype(jnp.bfloat16)).astype(jnp.float32).reshape(LEN, KVH, HD)
        query_norm = unit_rms(query_rows.astype(jnp.float32).reshape(LEN, QH, HD), q_gain.astype(jnp.float32))
        query_rot = lax.optimization_barrier(rotary(query_norm, row_pos, col_pos).astype(jnp.bfloat16)).astype(jnp.float32)
        key_norm = unit_rms(key_rows.astype(jnp.float32).reshape(LEN, KVH, HD), k_gain.astype(jnp.float32))
        key_rot = lax.optimization_barrier(rotary(key_norm, row_pos, col_pos).astype(jnp.bfloat16)).astype(jnp.float32)
        blocked = query_rot.reshape(LEN // block_rows, block_rows, KVH, group, HD)

        def one_block(query_block):
            scores = jnp.einsum('qkgd,nkd->kgqn', query_block, key_rot) * HD ** (-0.5)
            highest = lax.optimization_barrier(jnp.max(scores, axis=-1, keepdims=True))
            weights = jnp.exp(scores - highest)
            weights = weights / lax.optimization_barrier(jnp.sum(weights, axis=-1, keepdims=True))
            probability = lax.optimization_barrier(weights.astype(jnp.bfloat16)).astype(jnp.float32)
            blended = jnp.einsum('kgqn,nkd->qkgd', probability, values)
            return blended.astype(jnp.bfloat16).reshape(block_rows, QH * HD)
        return lax.map(one_block, blocked).reshape(LEN, QH * HD)
    return lax.map(one_sequence, (queries, keys, tokens))
```

```python
import functools
import math

import jax
import jax.numpy as jnp
import numpy as np
from jax import lax
from jax.experimental import pallas as pl
from jax.experimental.pallas import tpu as pltpu
from jax.sharding import PartitionSpec as P

HD = 128
QH = 16
KVH = 2
GRID_W = 64
GROUP = QH // KVH
epsilon = 1e-06
MESH = pl.DeviceIdType.MESH


def inner_size(n):
    size = 1
    while size * size * 4 <= n and n % (size * 2) == 0:
        size *= 2
    return size


def kernel(
    n_sp, n_dp, q_hbm, k_hbm, tok_hbm, w_hbm, qg_ref, kg_ref, freq_ref, out_hbm,
    q_in, k_in, tok, w_in, wbuf, kbuf, vbuf, qrot, prob, outbuf, cos_ref, sin_ref,
    in_sem, w_z, w_x, w_s, w_recv, w_srecv, k_send, k_recv, v_send, v_recv, v_fwd, v_frecv, out_sem,
):
    rows = q_hbm.shape[0]
    depth = w_hbm.shape[0]
    n_x = inner_size(n_dp)
    n_z = n_dp // n_x
    n_y = n_sp // 2
    sp = lax.axis_index("sp")
    dp = lax.axis_index("dp")
    z, x = dp // n_x, dp % n_x
    y, c = sp // 2, sp % 2
    sib = y * 2 + (1 - c)

    loads = [
        pltpu.make_async_copy(src, dst, in_sem.at[i])
        for i, (src, dst) in enumerate(
            ((w_hbm, w_in), (k_hbm, k_in), (q_hbm, q_in), (tok_hbm, tok))
        )
    ]
    for load in loads:
        load.start()

    z_peers = [((z + d) % n_z) for d in range(1, n_z)]
    x_peers = [((x + d) % n_x) for d in range(1, n_x)]
    sp_peers = [((sp + d) % n_sp) for d in range(1, n_sp)]
    y_peers = [((y + d) % n_y) for d in range(1, n_y)]

    barrier = pltpu.get_barrier_semaphore()
    for zp in z_peers:
        pl.semaphore_signal(barrier, inc=1, device_id=(sp, zp * n_x + x), device_id_type=MESH)
    for xp in x_peers:
        pl.semaphore_signal(barrier, inc=1, device_id=(sp, z * n_x + xp), device_id_type=MESH)
    for j in sp_peers:
        pl.semaphore_signal(barrier, inc=1, device_id=(j, dp), device_id_type=MESH)
    pl.semaphore_wait(barrier, n_z - 1 + n_x - 1 + n_sp - 1)

    pending = []

    def remote(src, dst, send, recv, where):
        return pltpu.make_async_remote_copy(
            src_ref=src, dst_ref=dst, send_sem=send, recv_sem=recv, device_id=where, device_id_type=MESH
        )

    def send(*args):
        copy = remote(*args)
        copy.start()
        pending.append(copy)

    def block(d, core):
        return wbuf.at[pl.ds(pl.multiple_of(d * depth, 16), depth), pl.ds(pl.multiple_of(core * HD, HD), HD)]

    mine = w_in.at[:, pl.ds(pl.multiple_of(c * HD, HD), HD)]
    loads[0].wait()
    for i, zp in enumerate(z_peers):
        send(mine, block(dp, c), w_z.at[i], w_recv.at[dp], (sp, zp * n_x + x))
    for i, xp in enumerate(x_peers):
        send(mine, block(dp, c), w_x.at[0, i], w_recv.at[dp], (sp, z * n_x + xp))

    pos = sp * rows + lax.broadcasted_iota(jnp.int32, (rows, HD), 0)
    lane = lax.broadcasted_iota(jnp.int32, (rows, HD), 1)
    grid_row = pos // GRID_W
    coord = jnp.where(lane < HD // 2, grid_row, pos - grid_row * GRID_W).astype(jnp.float32)
    angles = coord * freq_ref[...]
    first = lane % (HD // 2) < HD // 4
    cos_ref[...] = jnp.cos(angles)
    sine = jnp.sin(angles)
    sin_ref[...] = jnp.where(first, -sine, sine)

    def norm_rot(u, gain):
        u = u.astype(jnp.float32)
        u = u * lax.rsqrt(jnp.mean(u * u, axis=-1, keepdims=True) + epsilon) * gain
        other = jnp.where(first, pltpu.roll(u, HD - HD // 4, 1), pltpu.roll(u, HD // 4, 1))
        return (u * cos_ref[...] + other * sin_ref[...]).astype(jnp.bfloat16)

    def at(ref, s):
        return ref.at[pl.ds(pl.multiple_of(s * rows, 16), rows), :]

    own = pl.ds(pl.multiple_of(sp * rows, 16), rows)
    loads[1].wait()
    for g in range(KVH):
        kbuf[own, g * HD:(g + 1) * HD] = norm_rot(k_in[:, g * HD:(g + 1) * HD], kg_ref[...])
    for i, j in enumerate(sp_peers):
        send(at(kbuf, sp), at(kbuf, sp), k_send.at[i], k_recv.at[sp], (j, dp))

    wbuf[pl.ds(pl.multiple_of(dp * depth, 16), depth), :] = w_in[...]
    loads[2].wait()
    for h in range(QH):
        qrot[h] = norm_rot(q_in[:, h * HD:(h + 1) * HD], qg_ref[...])

    for j in sp_peers:
        remote(at(kbuf, j), at(kbuf, j), k_send.at[0], k_recv.at[j], (j, dp)).wait_recv()

    scale = HD ** -0.5 * math.log2(math.e)

    def weights(h, g):
        s = lax.dot_general(
            qrot[h], kbuf[:, g * HD:(g + 1) * HD], (((1,), (1,)), ((), ())),
            preferred_element_type=jnp.float32,
        )
        e = jnp.exp2((s - jnp.max(s, axis=-1, keepdims=True)) * scale)
        prob[h] = (e * (1.0 / jnp.sum(e, axis=-1, keepdims=True))).astype(jnp.bfloat16)

    def relay_z(i):
        d = z_peers[i] * n_x + x
        remote(block(d, c), block(d, c), w_z.at[0], w_recv.at[d], (sp, d)).wait_recv()
        for k, xp in enumerate(x_peers):
            send(block(d, c), block(d, c), w_x.at[i + 1, k], w_recv.at[d], (sp, z * n_x + xp))
        send(block(d, c), block(d, c), w_s.at[d], w_srecv.at[d], (sib, dp))

    def relay_x(zi, k):
        zz = z if zi < 0 else z_peers[zi]
        d = zz * n_x + x_peers[k]
        remote(block(d, c), block(d, c), w_z.at[0], w_recv.at[d], (sp, d)).wait_recv()
        send(block(d, c), block(d, c), w_s.at[d], w_srecv.at[d], (sib, dp))

    order = sorted(range(n_z - 1), key=lambda i: min(i + 1, n_z - 1 - i))
    relays = [functools.partial(relay_x, -1, k) for k in range(n_x - 1)]
    relays += [functools.partial(relay_z, i) for i in order]
    relays += [functools.partial(relay_x, i, k) for i in order for k in range(n_x - 1)]
    done = 0
    for part in range(GROUP // 2):
        count = len(relays) * (part + 1) // (GROUP // 2)
        for relay in relays[done:count]:
            relay()
        done = count
        for g in range(KVH):
            base = g * GROUP + part * 2

            @pl.loop(base, base + 2)
            def _(h, g=g):
                weights(h, g)

    for d in [z * n_x + xp for xp in x_peers] + [
        zp * n_x + xx for zp in z_peers for xx in [x] + x_peers
    ]:
        theirs = block(d, 1 - c)
        remote(theirs, theirs, w_s.at[0], w_srecv.at[d], (sib, dp)).wait_recv()

    loads[3].wait()
    vbuf[own, :] = jnp.dot(tok[...], wbuf[...], preferred_element_type=jnp.float32).astype(jnp.bfloat16)
    for i, yp in enumerate(y_peers):
        send(at(vbuf, sp), at(vbuf, sp), v_send.at[i], v_recv.at[sp], (yp * 2 + c, dp))
    send(at(vbuf, sp), at(vbuf, sp), v_send.at[n_y - 1], v_recv.at[sp], (sib, dp))
    for i, yp in enumerate(y_peers):
        j = yp * 2 + c
        remote(at(vbuf, j), at(vbuf, j), v_send.at[0], v_recv.at[j], (j, dp)).wait_recv()
        send(at(vbuf, j), at(vbuf, j), v_fwd.at[i], v_frecv.at[j], (sib, dp))
    remote(at(vbuf, sib), at(vbuf, sib), v_send.at[0], v_recv.at[sib], (sib, dp)).wait_recv()
    for yp in y_peers:
        j = yp * 2 + 1 - c
        remote(at(vbuf, j), at(vbuf, j), v_send.at[0], v_frecv.at[j], (sib, dp)).wait_recv()

    stores = []
    for part in range(4):
        for h in range(part * QH // 4, (part + 1) * QH // 4):
            g = h // GROUP
            outbuf[:, h * HD:(h + 1) * HD] = jnp.dot(
                prob[h], vbuf[:, g * HD:(g + 1) * HD], preferred_element_type=jnp.float32
            ).astype(jnp.bfloat16)
        cols = pl.ds(part * QH // 4 * HD, QH // 4 * HD)
        stores.append(pltpu.make_async_copy(outbuf.at[:, cols], out_hbm.at[:, cols], out_sem.at[part]))
        stores[-1].start()
    for copy in pending:
        copy.wait_send()
    for store in stores:
        store.wait()


def per_device(queries, keys, tokens, w_value, q_gain, k_gain):
    n_sp, n_dp = lax.axis_size("sp"), lax.axis_size("dp")
    n_x = inner_size(n_dp)
    n_z = n_dp // n_x
    n_y = n_sp // 2
    rows, width = tokens.shape[1:]
    depth = w_value.shape[0]
    quarter = HD // 4
    freq = 10000.0 ** (-jnp.arange(quarter, dtype=jnp.float32) * 2.0 / (HD // 2))
    freq = jnp.tile(freq, 4)[None]
    any_spec = pl.BlockSpec(memory_space=pl.ANY)
    vmem = pl.BlockSpec(memory_space=pltpu.VMEM)
    bf16 = jnp.bfloat16
    dma = pltpu.SemaphoreType.DMA
    out = pl.pallas_call(
        functools.partial(kernel, n_sp, n_dp),
        out_shape=jax.ShapeDtypeStruct((rows, QH * HD), bf16),
        in_specs=[any_spec] * 4 + [vmem] * 3,
        out_specs=any_spec,
        scratch_shapes=[
            pltpu.VMEM((rows, QH * HD), bf16),
            pltpu.VMEM((rows, KVH * HD), bf16),
            pltpu.VMEM((rows, width), bf16),
            pltpu.VMEM((depth, KVH * HD), bf16),
            pltpu.VMEM((width, KVH * HD), bf16),
            pltpu.VMEM((rows * n_sp, KVH * HD), bf16),
            pltpu.VMEM((rows * n_sp, KVH * HD), bf16),
            pltpu.VMEM((QH, rows, HD), bf16),
            pltpu.VMEM((QH, rows, rows * n_sp), bf16),
            pltpu.VMEM((rows, QH * HD), bf16),
            pltpu.VMEM((rows, HD), jnp.float32),
            pltpu.VMEM((rows, HD), jnp.float32),
            dma((4,)),
            dma((n_z,)),
            dma((n_z, n_x)),
            dma((n_dp,)),
            dma((n_dp,)),
            dma((n_dp,)),
            dma((n_sp,)),
            dma((n_sp,)),
            dma((n_y,)),
            dma((n_sp,)),
            dma((n_y,)),
            dma((n_sp,)),
            dma((4,)),
        ],
        compiler_params=pltpu.CompilerParams(
            collective_id=0, has_side_effects=True, vmem_limit_bytes=60 * 1024 * 1024
        ),
        name="fused_attention",
    )(queries[0], keys[0], tokens[0], w_value, q_gain[None], k_gain[None], freq)
    return out[None]


def solution(mesh):
    in_specs = (
        P("dp", "sp", None),
        P("dp", "sp", None),
        P("dp", "sp", None),
        P("dp", None),
        P(),
        P(),
    )
    return jax.shard_map(
        per_device, mesh=mesh, in_specs=in_specs, out_specs=P("dp", "sp", None), check_vma=False
    )
```

```python
import functools
import math

import jax
import jax.numpy as jnp
from jax import lax
from jax.experimental import pallas as pl
from jax.experimental.pallas import tpu as pltpu
from jax.sharding import PartitionSpec as P

HD = 128
QH = 16
KVH = 2
GRID_W = 64
GROUP = QH // KVH
epsilon = 1e-06
MESH = pl.DeviceIdType.MESH


def inner_size(n):
    size = 1
    while size * size * 4 <= n and n % (size * 2) == 0:
        size *= 2
    return size


def kernel(
    n_sp, n_dp, q_hbm, k_hbm, tok_hbm, w_hbm, qg_hbm, kg_hbm, out_ref,
    q_in, k_in, tok, wbuf, kbuf, vbuf, qrot, prob, cos_ref, sin_ref, qg_ref, kg_ref,
    in_sem, w_z, w_x, w_recv, t_send, t_recv, k_send, k_recv, k_fwd, k_frecv, v_send, v_recv, v_fwd, v_frecv,
):
    rows = q_hbm.shape[0]
    depth = w_hbm.shape[0]
    n_x = inner_size(n_dp)
    n_z = n_dp // n_x
    n_y = n_sp // 2
    sp = lax.axis_index("sp")
    dp = lax.axis_index("dp")
    z, x = dp // n_x, dp % n_x
    y, c = sp // 2, sp % 2
    sib = y * 2 + (1 - c)

    def block(d):
        return wbuf.at[pl.ds(pl.multiple_of(d * depth, 16), depth), :]

    def token_part(core):
        return tok.at[pl.ds(pl.multiple_of(core * rows, 16), rows), :]

    z_peers = [((z + d) % n_z) for d in range(1, n_z)]
    x_peers = [((x + d) % n_x) for d in range(1, n_x)]
    y_peers = [((y + d) % n_y) for d in range(1, n_y)]

    barrier = pltpu.get_barrier_semaphore()
    for zp in z_peers:
        pl.semaphore_signal(barrier, inc=1, device_id=(sp, zp * n_x + x), device_id_type=MESH)
    for xp in x_peers:
        pl.semaphore_signal(barrier, inc=1, device_id=(sp, z * n_x + xp), device_id_type=MESH)
    for yp in y_peers:
        pl.semaphore_signal(barrier, inc=1, device_id=(yp * 2 + c, dp), device_id_type=MESH)
    pl.semaphore_signal(barrier, inc=1, device_id=(sib, dp), device_id_type=MESH)

    w_mine = w_hbm.at[:, pl.ds(pl.multiple_of(c * HD, HD), HD)]
    loads = [
        pltpu.make_async_copy(src, dst, in_sem.at[i])
        for i, (src, dst) in enumerate(
            (
                (kg_hbm, kg_ref), (k_hbm, k_in), (w_mine, block(dp)), (tok_hbm, token_part(c)),
                (q_hbm, q_in), (qg_hbm, qg_ref),
            )
        )
    ]
    for load in loads:
        load.start()

    pending = []

    def remote(src, dst, send, recv, where):
        return pltpu.make_async_remote_copy(
            src_ref=src, dst_ref=dst, send_sem=send, recv_sem=recv, device_id=where, device_id_type=MESH
        )

    def send(*args):
        copy = remote(*args)
        copy.start()
        pending.append(copy)

    pos = sp * rows + lax.broadcasted_iota(jnp.int32, (rows, HD), 0)
    lane = lax.broadcasted_iota(jnp.int32, (rows, HD), 1)
    grid_row = pos // GRID_W
    coord = jnp.where(lane < HD // 2, grid_row, pos - grid_row * GRID_W).astype(jnp.float32)
    step = (lax.broadcasted_iota(jnp.int32, (1, HD), 1) % (HD // 4)).astype(jnp.float32)
    angles = coord * jnp.exp2(step * (-2.0 * math.log2(10000.0) / (HD // 2)))
    first = lane % (HD // 2) < HD // 4
    cos_ref[...] = jnp.cos(angles)
    sine = jnp.sin(angles)
    sin_ref[...] = jnp.where(first, -sine, sine)

    def norm_rot(u, gain):
        u = u.astype(jnp.float32)
        u = u * lax.rsqrt(jnp.mean(u * u, axis=-1, keepdims=True) + epsilon) * gain
        other = jnp.where(first, pltpu.roll(u, HD - HD // 4, 1), pltpu.roll(u, HD // 4, 1))
        return (u * cos_ref[...] + other * sin_ref[...]).astype(jnp.bfloat16)

    def at(ref, s):
        return ref.at[pl.ds(pl.multiple_of(s * rows, 16), rows), :]

    own = pl.ds(pl.multiple_of(sp * rows, 16), rows)
    loads[0].wait()
    loads[1].wait()
    for g in range(KVH):
        kbuf[own, g * HD:(g + 1) * HD] = norm_rot(k_in[:, g * HD:(g + 1) * HD], kg_ref[...])
    loads[2].wait()

    pl.semaphore_wait(barrier, n_z - 1 + n_x - 1 + n_y)
    for i, zp in enumerate(z_peers):
        send(block(dp), block(dp), w_z.at[i], w_recv.at[dp], (sp, zp * n_x + x))
    for i, xp in enumerate(x_peers):
        send(block(dp), block(dp), w_x.at[0, i], w_recv.at[dp], (sp, z * n_x + xp))
    for i, yp in enumerate(y_peers):
        send(at(kbuf, sp), at(kbuf, sp), k_send.at[i], k_recv.at[y], (yp * 2 + c, dp))
    send(at(kbuf, sp), at(kbuf, sp), k_send.at[n_y - 1], k_frecv.at[y], (sib, dp))
    loads[3].wait()
    send(token_part(c), token_part(c), t_send.at[0], t_recv.at[0], (sib, dp))

    loads[4].wait()
    loads[5].wait()
    for h in range(QH):
        qrot[h] = norm_rot(q_in[:, h * HD:(h + 1) * HD], qg_ref[...])

    for i, yp in enumerate(y_peers):
        j = yp * 2 + c
        remote(at(kbuf, j), at(kbuf, j), k_send.at[0], k_recv.at[yp], (j, dp)).wait_recv()
        send(at(kbuf, j), at(kbuf, j), k_fwd.at[i], k_frecv.at[yp], (sib, dp))
    for yp in [y] + y_peers:
        j = yp * 2 + 1 - c
        remote(at(kbuf, j), at(kbuf, j), k_send.at[0], k_frecv.at[yp], (sib, dp)).wait_recv()

    scale = HD ** -0.5 * math.log2(math.e)

    def weights(h, g):
        s = lax.dot_general(
            qrot[h], kbuf[:, g * HD:(g + 1) * HD], (((1,), (1,)), ((), ())),
            preferred_element_type=jnp.float32,
        )
        e = jnp.exp2((s - jnp.max(s, axis=-1, keepdims=True)) * scale)
        prob[h] = (e * (1.0 / jnp.sum(e, axis=-1, keepdims=True))).astype(jnp.bfloat16)

    def arrived(d):
        remote(block(d), block(d), w_z.at[0], w_recv.at[d], (sp, d)).wait_recv()

    def relay(i):
        d = z_peers[i] * n_x + x
        arrived(d)
        for k, xp in enumerate(x_peers):
            send(block(d), block(d), w_x.at[i + 1, k], w_recv.at[d], (sp, z * n_x + xp))

    order = sorted(range(n_z - 1), key=lambda i: min(i + 1, n_z - 1 - i))
    relays = [functools.partial(relay, i) for i in order]
    done = 0
    for part in range(GROUP // 2):
        count = len(relays) * (part + 1) // (GROUP // 2)
        for step_on in relays[done:count]:
            step_on()
        done = count
        for g in range(KVH):
            base = g * GROUP + part * 2

            @pl.loop(base, base + 2)
            def _(h, g=g):
                weights(h, g)

    for zz in [z] + [z_peers[i] for i in order]:
        for xp in x_peers:
            arrived(zz * n_x + xp)
    theirs = token_part(1 - c)
    remote(theirs, theirs, t_send.at[0], t_recv.at[0], (sib, dp)).wait_recv()

    def chip(head, yy):
        return vbuf.at[head, pl.ds(pl.multiple_of(yy * 2 * rows, 16), 2 * rows), :]

    chip(c, y)[...] = jnp.dot(tok[...], wbuf[...], preferred_element_type=jnp.float32).astype(jnp.bfloat16)
    for i, yp in enumerate(y_peers):
        send(chip(c, y), chip(c, y), v_send.at[i], v_recv.at[y], (yp * 2 + c, dp))
    send(chip(c, y), chip(c, y), v_send.at[n_y - 1], v_frecv.at[y], (sib, dp))
    for i, yp in enumerate(y_peers):
        there = chip(c, yp)
        remote(there, there, v_send.at[0], v_recv.at[yp], (yp * 2 + c, dp)).wait_recv()
        send(there, there, v_fwd.at[i], v_frecv.at[yp], (sib, dp))
    for yp in [y] + y_peers:
        there = chip(1 - c, yp)
        remote(there, there, v_send.at[0], v_frecv.at[yp], (sib, dp)).wait_recv()

    for h in range(QH):
        out_ref[:, h * HD:(h + 1) * HD] = jnp.dot(
            prob[h], vbuf[h // GROUP], preferred_element_type=jnp.float32
        ).astype(jnp.bfloat16)
    for copy in pending:
        copy.wait_send()


def per_device(queries, keys, tokens, w_value, q_gain, k_gain):
    n_sp, n_dp = lax.axis_size("sp"), lax.axis_size("dp")
    n_x = inner_size(n_dp)
    n_z = n_dp // n_x
    n_y = n_sp // 2
    rows, width = tokens.shape[1:]
    depth = w_value.shape[0]
    any_spec = pl.BlockSpec(memory_space=pltpu.HBM)
    bf16, f32 = jnp.bfloat16, jnp.float32
    dma = pltpu.SemaphoreType.DMA
    length = rows * n_sp
    buffers = [
        ((rows, QH * HD), bf16),
        ((rows, KVH * HD), bf16),
        ((2 * rows, width), bf16),
        ((width, HD), bf16),
        ((length, KVH * HD), bf16),
        ((KVH, length, HD), bf16),
        ((QH, rows, HD), bf16),
        ((QH, rows, length), bf16),
        ((rows, HD), f32),
        ((rows, HD), f32),
        ((1, HD), f32),
        ((1, HD), f32),
    ]
    held = sum(math.prod(shape) * jnp.dtype(kind).itemsize for shape, kind in buffers)
    limit = min(60 * 2 ** 20, held + held // 4 + 8 * rows * length * 4 + 4 * 2 ** 20)
    out = pl.pallas_call(
        functools.partial(kernel, n_sp, n_dp),
        out_shape=jax.ShapeDtypeStruct((rows, QH * HD), bf16),
        in_specs=[any_spec] * 6,
        out_specs=pl.BlockSpec(memory_space=pltpu.VMEM),
        scratch_shapes=[pltpu.VMEM(shape, kind) for shape, kind in buffers]
        + [
            dma((6,)),
            dma((n_z,)),
            dma((n_z, n_x)),
            dma((n_dp,)),
            dma((1,)),
            dma((1,)),
            dma((n_y,)),
            dma((n_y,)),
            dma((n_y,)),
            dma((n_y,)),
            dma((n_y,)),
            dma((n_y,)),
            dma((n_y,)),
            dma((n_y,)),
        ],
        compiler_params=pltpu.CompilerParams(
            collective_id=0, has_side_effects=True, vmem_limit_bytes=limit
        ),
        name="fused_attention",
    )(queries[0], keys[0], tokens[0], w_value, q_gain[None], k_gain[None])
    return out[None]


def solution(mesh):
    in_specs = (
        P("dp", "sp", None),
        P("dp", "sp", None),
        P("dp", "sp", None),
        P("dp", None),
        P(),
        P(),
    )
    return jax.shard_map(
        per_device, mesh=mesh, in_specs=in_specs, out_specs=P("dp", "sp", None), check_vma=False
    )
```

```python
import functools
import math

import jax
import jax.numpy as jnp
from jax import lax
from jax.experimental import pallas as pl
from jax.experimental.pallas import tpu as pltpu
from jax.sharding import PartitionSpec as P

HD = 128
QH = 16
KVH = 2
GRID_W = 64
GROUP = QH // KVH
epsilon = 1e-06
MESH = pl.DeviceIdType.MESH


def inner_size(n):
    size = 1
    while size * size * 4 <= n and n % (size * 2) == 0:
        size *= 2
    return size


def kernel(
    n_sp, n_dp, q_hbm, k_hbm, tok_hbm, w_hbm, qg_hbm, kg_hbm, out_ref,
    q_in, k_in, tok, wbuf, kbuf, vbuf, qrot, prob, cos_ref, sin_ref, qg_ref, kg_ref,
    in_sem, w_z, w_x, w_recv, t_send, t_recv, k_send, k_recv, k_fwd, k_frecv, v_send, v_recv, v_fwd, v_frecv,
):
    rows = q_hbm.shape[0]
    depth = w_hbm.shape[0]
    n_x = inner_size(n_dp)
    n_z = n_dp // n_x
    n_y = n_sp // 2
    sp = lax.axis_index("sp")
    dp = lax.axis_index("dp")
    z, x = dp // n_x, dp % n_x
    y, c = sp // 2, sp % 2
    sib = y * 2 + (1 - c)

    def block(d):
        return wbuf.at[pl.ds(pl.multiple_of(d * depth, 16), depth), :]

    def token_part(core):
        return tok.at[pl.ds(pl.multiple_of(core * rows, 16), rows), :]

    z_peers = [((z + d) % n_z) for d in range(1, n_z)]
    x_peers = [((x + d) % n_x) for d in range(1, n_x)]
    y_peers = [((y + d) % n_y) for d in range(1, n_y)]

    barrier = pltpu.get_barrier_semaphore()
    for zp in z_peers:
        pl.semaphore_signal(barrier, inc=1, device_id=(sp, zp * n_x + x), device_id_type=MESH)
    for xp in x_peers:
        pl.semaphore_signal(barrier, inc=1, device_id=(sp, z * n_x + xp), device_id_type=MESH)
    for yp in y_peers:
        pl.semaphore_signal(barrier, inc=1, device_id=(yp * 2 + c, dp), device_id_type=MESH)
    pl.semaphore_signal(barrier, inc=1, device_id=(sib, dp), device_id_type=MESH)

    w_mine = w_hbm.at[:, pl.ds(pl.multiple_of(c * HD, HD), HD)]
    loads = [
        pltpu.make_async_copy(src, dst, in_sem.at[i])
        for i, (src, dst) in enumerate(
            (
                (kg_hbm, kg_ref), (k_hbm, k_in), (w_mine, block(dp)), (tok_hbm, token_part(c)),
                (q_hbm, q_in), (qg_hbm, qg_ref),
            )
        )
    ]
    for load in loads:
        load.start()

    pending = []

    def remote(src, dst, send, recv, where):
        return pltpu.make_async_remote_copy(
            src_ref=src, dst_ref=dst, send_sem=send, recv_sem=recv, device_id=where, device_id_type=MESH
        )

    def send(*args):
        copy = remote(*args)
        copy.start()
        pending.append(copy)

    pos = sp * rows + lax.broadcasted_iota(jnp.int32, (rows, HD), 0)
    lane = lax.broadcasted_iota(jnp.int32, (rows, HD), 1)
    grid_row = pos // GRID_W
    coord = jnp.where(lane < HD // 2, grid_row, pos - grid_row * GRID_W).astype(jnp.float32)
    step = (lax.broadcasted_iota(jnp.int32, (1, HD), 1) % (HD // 4)).astype(jnp.float32)
    angles = coord * jnp.exp2(step * (-2.0 * math.log2(10000.0) / (HD // 2)))
    first = lane % (HD // 2) < HD // 4
    cos_ref[...] = jnp.cos(angles)
    sine = jnp.sin(angles)
    sin_ref[...] = jnp.where(first, -sine, sine)

    def norm_rot(u, gain):
        u = u.astype(jnp.float32)
        u = u * lax.rsqrt(jnp.mean(u * u, axis=-1, keepdims=True) + epsilon) * gain
        other = jnp.where(first, pltpu.roll(u, HD - HD // 4, 1), pltpu.roll(u, HD // 4, 1))
        return (u * cos_ref[...] + other * sin_ref[...]).astype(jnp.bfloat16)

    def at(ref, s):
        return ref.at[pl.ds(pl.multiple_of(s * rows, 16), rows), :]

    own = pl.ds(pl.multiple_of(sp * rows, 16), rows)
    loads[0].wait()
    loads[1].wait()
    for g in range(KVH):
        kbuf[own, g * HD:(g + 1) * HD] = norm_rot(k_in[:, g * HD:(g + 1) * HD], kg_ref[...])
    loads[2].wait()

    pl.semaphore_wait(barrier, n_z - 1 + n_x - 1 + n_y)
    for i, zp in enumerate(z_peers):
        send(block(dp), block(dp), w_z.at[i], w_recv.at[dp], (sp, zp * n_x + x))
    for i, xp in enumerate(x_peers):
        send(block(dp), block(dp), w_x.at[0, i], w_recv.at[dp], (sp, z * n_x + xp))
    for i, yp in enumerate(y_peers):
        send(at(kbuf, sp), at(kbuf, sp), k_send.at[i], k_recv.at[y], (yp * 2 + c, dp))
    send(at(kbuf, sp), at(kbuf, sp), k_send.at[n_y - 1], k_frecv.at[y], (sib, dp))
    loads[3].wait()
    send(token_part(c), token_part(c), t_send.at[0], t_recv.at[0], (sib, dp))

    loads[4].wait()
    loads[5].wait()
    for h in range(QH):
        qrot[h] = norm_rot(q_in[:, h * HD:(h + 1) * HD], qg_ref[...])

    for i, yp in enumerate(y_peers):
        j = yp * 2 + c
        remote(at(kbuf, j), at(kbuf, j), k_send.at[0], k_recv.at[yp], (j, dp)).wait_recv()
        send(at(kbuf, j), at(kbuf, j), k_fwd.at[i], k_frecv.at[yp], (sib, dp))
    for yp in [y] + y_peers:
        j = yp * 2 + 1 - c
        remote(at(kbuf, j), at(kbuf, j), k_send.at[0], k_frecv.at[yp], (sib, dp)).wait_recv()

    scale = HD ** -0.5 * math.log2(math.e)

    def weights(h, g):
        s = lax.dot_general(
            qrot[h], kbuf[:, g * HD:(g + 1) * HD], (((1,), (1,)), ((), ())),
            preferred_element_type=jnp.float32,
        )
        e = jnp.exp2((s - jnp.max(s, axis=-1, keepdims=True)) * scale)
        prob[h] = (e * (1.0 / jnp.sum(e, axis=-1, keepdims=True))).astype(jnp.bfloat16)

    def arrived(d):
        remote(block(d), block(d), w_z.at[0], w_recv.at[d], (sp, d)).wait_recv()

    def relay(i):
        d = z_peers[i] * n_x + x
        arrived(d)
        for k, xp in enumerate(x_peers):
            send(block(d), block(d), w_x.at[i + 1, k], w_recv.at[d], (sp, z * n_x + xp))

    order = sorted(range(n_z - 1), key=lambda i: min(i + 1, n_z - 1 - i))
    relays = [functools.partial(relay, i) for i in order]
    done = 0
    for part in range(GROUP // 2):
        count = len(relays) * (part + 1) // (GROUP // 2)
        for step_on in relays[done:count]:
            step_on()
        done = count
        for g in range(KVH):
            base = g * GROUP + part * 2

            @pl.loop(base, base + 2)
            def _(h, g=g):
                weights(h, g)

    for zz in [z] + [z_peers[i] for i in order]:
        for xp in x_peers:
            arrived(zz * n_x + xp)
    theirs = token_part(1 - c)
    remote(theirs, theirs, t_send.at[0], t_recv.at[0], (sib, dp)).wait_recv()

    def chip(head, yy):
        return vbuf.at[head, pl.ds(pl.multiple_of(yy * 2 * rows, 16), 2 * rows), :]

    chip(c, y)[...] = jnp.dot(tok[...], wbuf[...], preferred_element_type=jnp.float32).astype(jnp.bfloat16)
    for i, yp in enumerate(y_peers):
        send(chip(c, y), chip(c, y), v_send.at[i], v_recv.at[y], (yp * 2 + c, dp))
    send(chip(c, y), chip(c, y), v_send.at[n_y - 1], v_frecv.at[y], (sib, dp))
    for i, yp in enumerate(y_peers):
        there = chip(c, yp)
        remote(there, there, v_send.at[0], v_recv.at[yp], (yp * 2 + c, dp)).wait_recv()
        send(there, there, v_fwd.at[i], v_frecv.at[yp], (sib, dp))
    for yp in [y] + y_peers:
        there = chip(1 - c, yp)
        remote(there, there, v_send.at[0], v_frecv.at[yp], (sib, dp)).wait_recv()

    for h in range(QH):
        out_ref[:, h * HD:(h + 1) * HD] = jnp.dot(
            prob[h], vbuf[h // GROUP], preferred_element_type=jnp.float32
        ).astype(jnp.bfloat16)
    for copy in pending:
        copy.wait_send()


def per_device(queries, keys, tokens, w_value, q_gain, k_gain):
    n_sp, n_dp = lax.axis_size("sp"), lax.axis_size("dp")
    n_x = inner_size(n_dp)
    n_z = n_dp // n_x
    n_y = n_sp // 2
    rows, width = tokens.shape[1:]
    depth = w_value.shape[0]
    any_spec = pl.BlockSpec(memory_space=pltpu.HBM)
    bf16, f32 = jnp.bfloat16, jnp.float32
    dma = pltpu.SemaphoreType.DMA
    length = rows * n_sp
    buffers = [
        ((rows, QH * HD), bf16),
        ((rows, KVH * HD), bf16),
        ((2 * rows, width), bf16),
        ((width, HD), bf16),
        ((length, KVH * HD), bf16),
        ((KVH, length, HD), bf16),
        ((QH, rows, HD), bf16),
        ((QH, rows, length), bf16),
        ((rows, HD), f32),
        ((rows, HD), f32),
        ((1, HD), f32),
        ((1, HD), f32),
    ]
    held = sum(math.prod(shape) * jnp.dtype(kind).itemsize for shape, kind in buffers)
    limit = min(60 * 2 ** 20, held + held // 4 + 8 * rows * length * 4 + 4 * 2 ** 20)
    operands = (queries[0], keys[0], tokens[0], w_value, q_gain[None], k_gain[None])
    operands = [pltpu.with_memory_space_constraint(a, pltpu.HBM) for a in operands]
    out = pl.pallas_call(
        functools.partial(kernel, n_sp, n_dp),
        out_shape=jax.ShapeDtypeStruct((rows, QH * HD), bf16),
        in_specs=[any_spec] * 6,
        out_specs=pl.BlockSpec(memory_space=pltpu.VMEM),
        scratch_shapes=[pltpu.VMEM(shape, kind) for shape, kind in buffers]
        + [
            dma((6,)),
            dma((n_z,)),
            dma((n_z, n_x)),
            dma((n_dp,)),
            dma((1,)),
            dma((1,)),
            dma((n_y,)),
            dma((n_y,)),
            dma((n_y,)),
            dma((n_y,)),
            dma((n_y,)),
            dma((n_y,)),
            dma((n_y,)),
            dma((n_y,)),
        ],
        compiler_params=pltpu.CompilerParams(
            collective_id=0, has_side_effects=True, vmem_limit_bytes=limit
        ),
        name="fused_attention",
    )(*operands)
    return out[None]


def solution(mesh):
    in_specs = (
        P("dp", "sp", None),
        P("dp", "sp", None),
        P("dp", "sp", None),
        P("dp", None),
        P(),
        P(),
    )
    return jax.shard_map(
        per_device, mesh=mesh, in_specs=in_specs, out_specs=P("dp", "sp", None), check_vma=False
    )
```

```python
import functools
import math

import jax
import jax.numpy as jnp
from jax import lax
from jax.experimental import pallas as pl
from jax.experimental.pallas import tpu as pltpu
from jax.sharding import PartitionSpec as P

HD = 128
QH = 16
KVH = 2
GRID_W = 64
GROUP = QH // KVH
epsilon = 1e-06
MESH = pl.DeviceIdType.MESH


def inner_size(n):
    size = 1
    while size * size * 4 <= n and n % (size * 2) == 0:
        size *= 2
    return size


def partner(index, d, n):
    if n & (n - 1):
        return (index + d) % n
    bit = 1
    while bit <= d:
        if d & bit:
            index = index + bit - 2 * bit * (index // bit % 2)
        bit *= 2
    return index


def kernel(
    n_sp, n_dp, q_hbm, k_hbm, tok_hbm, w_hbm, qg_hbm, kg_hbm, out_ref,
    q_in, k_in, tok, wbuf, kbuf, vbuf, qrot, prob, cos_ref, sin_ref, qg_ref, kg_ref,
    in_sem, w_z, w_x, w_recv, t_send, t_recv, k_send, k_recv, k_fwd, k_frecv, v_send, v_recv, v_fwd, v_frecv,
):
    rows = q_hbm.shape[0]
    depth = w_hbm.shape[0]
    n_x = inner_size(n_dp)
    n_z = n_dp // n_x
    n_y = n_sp // 2
    sp = lax.axis_index("sp")
    dp = lax.axis_index("dp")
    z, x = dp // n_x, dp % n_x
    y, c = sp // 2, sp % 2
    sib = y * 2 + (1 - c)

    def block(d):
        return wbuf.at[pl.ds(pl.multiple_of(d * depth, 16), depth), :]

    def token_part(core):
        return tok.at[pl.ds(pl.multiple_of(core * rows, 16), rows), :]

    z_peers = [partner(z, d, n_z) for d in range(1, n_z)]
    x_peers = [((x + d) % n_x) for d in range(1, n_x)]
    y_peers = [((y + d) % n_y) for d in range(1, n_y)]

    barrier = pltpu.get_barrier_semaphore()
    for zp in z_peers:
        pl.semaphore_signal(barrier, inc=1, device_id=(sp, zp * n_x + x), device_id_type=MESH)
    for xp in x_peers:
        pl.semaphore_signal(barrier, inc=1, device_id=(sp, z * n_x + xp), device_id_type=MESH)
    for yp in y_peers:
        pl.semaphore_signal(barrier, inc=1, device_id=(yp * 2 + c, dp), device_id_type=MESH)
    pl.semaphore_signal(barrier, inc=1, device_id=(sib, dp), device_id_type=MESH)

    w_mine = w_hbm.at[:, pl.ds(pl.multiple_of(c * HD, HD), HD)]
    loads = [
        pltpu.make_async_copy(src, dst, in_sem.at[i])
        for i, (src, dst) in enumerate(
            (
                (kg_hbm, kg_ref), (k_hbm, k_in), (w_mine, block(dp)), (tok_hbm, token_part(c)),
                (q_hbm, q_in), (qg_hbm, qg_ref),
            )
        )
    ]
    for load in loads:
        load.start()

    pending = []

    def remote(src, dst, send, recv, where):
        return pltpu.make_async_remote_copy(
            src_ref=src, dst_ref=dst, send_sem=send, recv_sem=recv, device_id=where, device_id_type=MESH
        )

    def send(*args):
        copy = remote(*args)
        copy.start()
        pending.append(copy)

    pos = sp * rows + lax.broadcasted_iota(jnp.int32, (rows, HD), 0)
    lane = lax.broadcasted_iota(jnp.int32, (rows, HD), 1)
    grid_row = pos // GRID_W
    coord = jnp.where(lane < HD // 2, grid_row, pos - grid_row * GRID_W).astype(jnp.float32)
    step = (lax.broadcasted_iota(jnp.int32, (1, HD), 1) % (HD // 4)).astype(jnp.float32)
    angles = coord * jnp.exp2(step * (-2.0 * math.log2(10000.0) / (HD // 2)))
    first = lane % (HD // 2) < HD // 4
    cos_ref[...] = jnp.cos(angles)
    sine = jnp.sin(angles)
    sin_ref[...] = jnp.where(first, -sine, sine)

    def norm_rot(u, gain):
        u = u.astype(jnp.float32)
        u = u * lax.rsqrt(jnp.mean(u * u, axis=-1, keepdims=True) + epsilon) * gain
        other = jnp.where(first, pltpu.roll(u, HD - HD // 4, 1), pltpu.roll(u, HD // 4, 1))
        return (u * cos_ref[...] + other * sin_ref[...]).astype(jnp.bfloat16)

    def at(ref, s):
        return ref.at[pl.ds(pl.multiple_of(s * rows, 16), rows), :]

    own = pl.ds(pl.multiple_of(sp * rows, 16), rows)
    loads[0].wait()
    loads[1].wait()
    for g in range(KVH):
        kbuf[own, g * HD:(g + 1) * HD] = norm_rot(k_in[:, g * HD:(g + 1) * HD], kg_ref[...])
    loads[2].wait()

    pl.semaphore_wait(barrier, n_z - 1 + n_x - 1 + n_y)
    for i, zp in enumerate(z_peers):
        send(block(dp), block(dp), w_z.at[i], w_recv.at[dp], (sp, zp * n_x + x))
    for i, xp in enumerate(x_peers):
        send(block(dp), block(dp), w_x.at[0, i], w_recv.at[dp], (sp, z * n_x + xp))
    for i, yp in enumerate(y_peers):
        send(at(kbuf, sp), at(kbuf, sp), k_send.at[i], k_recv.at[y], (yp * 2 + c, dp))
    send(at(kbuf, sp), at(kbuf, sp), k_send.at[n_y - 1], k_frecv.at[y], (sib, dp))
    loads[3].wait()
    send(token_part(c), token_part(c), t_send.at[0], t_recv.at[0], (sib, dp))

    loads[4].wait()
    loads[5].wait()
    for h in range(QH):
        qrot[h] = norm_rot(q_in[:, h * HD:(h + 1) * HD], qg_ref[...])

    def arrived(d):
        remote(block(d), block(d), w_z.at[0], w_recv.at[d], (sp, d)).wait_recv()

    def relay(i):
        d = z_peers[i] * n_x + x
        arrived(d)
        for k, xp in enumerate(x_peers):
            send(block(d), block(d), w_x.at[i + 1, k], w_recv.at[d], (sp, z * n_x + xp))

    relays = [functools.partial(relay, i) for i in range(n_z - 1)]
    for i, yp in enumerate(y_peers):
        j = yp * 2 + c
        remote(at(kbuf, j), at(kbuf, j), k_send.at[0], k_recv.at[yp], (j, dp)).wait_recv()
        send(at(kbuf, j), at(kbuf, j), k_fwd.at[i], k_frecv.at[yp], (sib, dp))
    for step_on in relays[:1]:
        step_on()
    for yp in [y] + y_peers:
        j = yp * 2 + 1 - c
        remote(at(kbuf, j), at(kbuf, j), k_send.at[0], k_frecv.at[yp], (sib, dp)).wait_recv()

    scale = HD ** -0.5 * math.log2(math.e)

    def weights(h, g):
        s = lax.dot_general(
            qrot[h], kbuf[:, g * HD:(g + 1) * HD], (((1,), (1,)), ((), ())),
            preferred_element_type=jnp.float32,
        )
        e = jnp.exp2((s - jnp.max(s, axis=-1, keepdims=True)) * scale)
        prob[h] = (e * (1.0 / jnp.sum(e, axis=-1, keepdims=True))).astype(jnp.bfloat16)

    relays = relays[1:]
    done = 0
    for part in range(GROUP // 2):
        count = len(relays) * part // (GROUP // 2 - 1) if part != 1 else -(-len(relays) // 2)
        for step_on in relays[done:count]:
            step_on()
        done = count
        for g in range(KVH):
            base = g * GROUP + part * 2

            @pl.loop(base, base + 2)
            def _(h, g=g):
                weights(h, g)

    for zz in [z] + z_peers:
        for xp in x_peers:
            arrived(zz * n_x + xp)
    theirs = token_part(1 - c)
    remote(theirs, theirs, t_send.at[0], t_recv.at[0], (sib, dp)).wait_recv()

    def chip(head, yy):
        return vbuf.at[head, pl.ds(pl.multiple_of(yy * 2 * rows, 16), 2 * rows), :]

    chip(c, y)[...] = jnp.dot(tok[...], wbuf[...], preferred_element_type=jnp.float32).astype(jnp.bfloat16)
    for i, yp in enumerate(y_peers):
        send(chip(c, y), chip(c, y), v_send.at[i], v_recv.at[y], (yp * 2 + c, dp))
    send(chip(c, y), chip(c, y), v_send.at[n_y - 1], v_frecv.at[y], (sib, dp))
    for i, yp in enumerate(y_peers):
        there = chip(c, yp)
        remote(there, there, v_send.at[0], v_recv.at[yp], (yp * 2 + c, dp)).wait_recv()
        send(there, there, v_fwd.at[i], v_frecv.at[yp], (sib, dp))

    def attend(core):
        for i in range(GROUP):
            h = core * GROUP + i
            out_ref[:, pl.ds(pl.multiple_of(h * HD, HD), HD)] = jnp.dot(
                prob[h], vbuf[core], preferred_element_type=jnp.float32
            ).astype(jnp.bfloat16)

    attend(c)
    for yp in [y] + y_peers:
        there = chip(1 - c, yp)
        remote(there, there, v_send.at[0], v_frecv.at[yp], (sib, dp)).wait_recv()
    attend(1 - c)
    for copy in pending:
        copy.wait_send()


def per_device(queries, keys, tokens, w_value, q_gain, k_gain):
    n_sp, n_dp = lax.axis_size("sp"), lax.axis_size("dp")
    n_x = inner_size(n_dp)
    n_z = n_dp // n_x
    n_y = n_sp // 2
    rows, width = tokens.shape[1:]
    depth = w_value.shape[0]
    any_spec = pl.BlockSpec(memory_space=pltpu.HBM)
    bf16, f32 = jnp.bfloat16, jnp.float32
    dma = pltpu.SemaphoreType.DMA
    length = rows * n_sp
    buffers = [
        ((rows, QH * HD), bf16),
        ((rows, KVH * HD), bf16),
        ((2 * rows, width), bf16),
        ((width, HD), bf16),
        ((length, KVH * HD), bf16),
        ((KVH, length, HD), bf16),
        ((QH, rows, HD), bf16),
        ((QH, rows, length), bf16),
        ((rows, HD), f32),
        ((rows, HD), f32),
        ((1, HD), f32),
        ((1, HD), f32),
    ]
    held = sum(math.prod(shape) * jnp.dtype(kind).itemsize for shape, kind in buffers)
    limit = min(60 * 2 ** 20, held + held // 4 + 8 * rows * length * 4 + 4 * 2 ** 20)
    operands = (queries[0], keys[0], tokens[0], w_value, q_gain[None], k_gain[None])
    operands = [pltpu.with_memory_space_constraint(a, pltpu.HBM) for a in operands]
    out = pl.pallas_call(
        functools.partial(kernel, n_sp, n_dp),
        out_shape=jax.ShapeDtypeStruct((rows, QH * HD), bf16),
        in_specs=[any_spec] * 6,
        out_specs=pl.BlockSpec(memory_space=pltpu.VMEM),
        scratch_shapes=[pltpu.VMEM(shape, kind) for shape, kind in buffers]
        + [
            dma((6,)),
            dma((n_z,)),
            dma((n_z, n_x)),
            dma((n_dp,)),
            dma((1,)),
            dma((1,)),
            dma((n_y,)),
            dma((n_y,)),
            dma((n_y,)),
            dma((n_y,)),
            dma((n_y,)),
            dma((n_y,)),
            dma((n_y,)),
            dma((n_y,)),
        ],
        compiler_params=pltpu.CompilerParams(
            collective_id=0, has_side_effects=True, vmem_limit_bytes=limit
        ),
        name="fused_attention",
    )(*operands)
    return out[None]


def solution(mesh):
    in_specs = (
        P("dp", "sp", None),
        P("dp", "sp", None),
        P("dp", "sp", None),
        P("dp", None),
        P(),
        P(),
    )
    return jax.shard_map(
        per_device, mesh=mesh, in_specs=in_specs, out_specs=P("dp", "sp", None), check_vma=False
    )
```

```python
import functools
import math

import jax
import jax.numpy as jnp
from jax import lax
from jax.experimental import pallas as pl
from jax.experimental.pallas import tpu as pltpu
from jax.sharding import PartitionSpec as P

HD = 128
QH = 16
KVH = 2
GRID_W = 64
GROUP = QH // KVH
epsilon = 1e-06
MESH = pl.DeviceIdType.MESH


def inner_size(n):
    size = 1
    while size * size * 4 <= n and n % (size * 2) == 0:
        size *= 2
    return size


def partner(index, d, n):
    if n & (n - 1):
        return (index + d) % n
    bit = 1
    while bit <= d:
        if d & bit:
            index = index + bit - 2 * bit * (index // bit % 2)
        bit *= 2
    return index


def kernel(
    n_sp, n_dp, q_hbm, k_hbm, tok_hbm, w_hbm, qg_hbm, kg_hbm, out_ref,
    q_in, k_in, tok, wbuf, kbuf, vbuf, qrot, prob, cos_ref, sin_ref, qg_ref, kg_ref,
    in_sem, w_z, w_x, w_recv, t_send, t_recv, k_send, k_recv, k_fwd, k_frecv, v_send, v_recv, v_fwd, v_frecv,
):
    rows = q_hbm.shape[0]
    depth = w_hbm.shape[0]
    n_x = inner_size(n_dp)
    n_z = n_dp // n_x
    n_y = n_sp // 2
    sp = lax.axis_index("sp")
    dp = lax.axis_index("dp")
    z, x = dp // n_x, dp % n_x
    y, c = sp // 2, sp % 2
    sib = y * 2 + (1 - c)

    def block(d):
        return wbuf.at[pl.ds(pl.multiple_of(d * depth, 16), depth), :]

    def token_part(core):
        return tok.at[pl.ds(pl.multiple_of(core * rows, 16), rows), :]

    z_peers = [partner(z, d, n_z) for d in range(1, n_z)]
    x_peers = [((x + d) % n_x) for d in range(1, n_x)]
    y_peers = [((y + d) % n_y) for d in range(1, n_y)]

    barrier = pltpu.get_barrier_semaphore()
    for zp in z_peers:
        pl.semaphore_signal(barrier, inc=1, device_id=(sp, zp * n_x + x), device_id_type=MESH)
    for xp in x_peers:
        pl.semaphore_signal(barrier, inc=1, device_id=(sp, z * n_x + xp), device_id_type=MESH)
    for yp in y_peers:
        pl.semaphore_signal(barrier, inc=1, device_id=(yp * 2 + c, dp), device_id_type=MESH)
    pl.semaphore_signal(barrier, inc=1, device_id=(sib, dp), device_id_type=MESH)

    w_mine = w_hbm.at[:, pl.ds(pl.multiple_of(c * HD, HD), HD)]
    loads = [
        pltpu.make_async_copy(src, dst, in_sem.at[i])
        for i, (src, dst) in enumerate(
            (
                (kg_hbm, kg_ref), (k_hbm, k_in), (w_mine, block(dp)), (tok_hbm, token_part(c)),
                (q_hbm, q_in), (qg_hbm, qg_ref),
            )
        )
    ]
    for load in loads:
        load.start()

    pending = []

    def remote(src, dst, send, recv, where):
        return pltpu.make_async_remote_copy(
            src_ref=src, dst_ref=dst, send_sem=send, recv_sem=recv, device_id=where, device_id_type=MESH
        )

    def send(*args):
        copy = remote(*args)
        copy.start()
        pending.append(copy)

    pos = sp * rows + lax.broadcasted_iota(jnp.int32, (rows, HD), 0)
    lane = lax.broadcasted_iota(jnp.int32, (rows, HD), 1)
    grid_row = pos // GRID_W
    coord = jnp.where(lane < HD // 2, grid_row, pos - grid_row * GRID_W).astype(jnp.float32)
    step = (lax.broadcasted_iota(jnp.int32, (1, HD), 1) % (HD // 4)).astype(jnp.float32)
    angles = coord * jnp.exp2(step * (-2.0 * math.log2(10000.0) / (HD // 2)))
    first = lane % (HD // 2) < HD // 4
    cos_ref[...] = jnp.cos(angles)
    sine = jnp.sin(angles)
    sin_ref[...] = jnp.where(first, -sine, sine)

    def norm_rot(u, gain):
        u = u.astype(jnp.float32)
        u = u * lax.rsqrt(jnp.mean(u * u, axis=-1, keepdims=True) + epsilon) * gain
        other = jnp.where(first, pltpu.roll(u, HD - HD // 4, 1), pltpu.roll(u, HD // 4, 1))
        return (u * cos_ref[...] + other * sin_ref[...]).astype(jnp.bfloat16)

    def at(ref, s):
        return ref.at[pl.ds(pl.multiple_of(s * rows, 16), rows), :]

    own = pl.ds(pl.multiple_of(sp * rows, 16), rows)
    loads[2].wait()

    pl.semaphore_wait(barrier, n_z - 1 + n_x - 1 + n_y)
    for i, zp in enumerate(z_peers):
        send(block(dp), block(dp), w_z.at[i], w_recv.at[dp], (sp, zp * n_x + x))
    for i, xp in enumerate(x_peers):
        send(block(dp), block(dp), w_x.at[0, i], w_recv.at[dp], (sp, z * n_x + xp))
    loads[0].wait()
    loads[1].wait()
    for g in range(KVH):
        kbuf[own, g * HD:(g + 1) * HD] = norm_rot(k_in[:, g * HD:(g + 1) * HD], kg_ref[...])
    for i, yp in enumerate(y_peers):
        send(at(kbuf, sp), at(kbuf, sp), k_send.at[i], k_recv.at[y], (yp * 2 + c, dp))
    send(at(kbuf, sp), at(kbuf, sp), k_send.at[n_y - 1], k_frecv.at[y], (sib, dp))
    loads[3].wait()
    send(token_part(c), token_part(c), t_send.at[0], t_recv.at[0], (sib, dp))

    loads[4].wait()
    loads[5].wait()
    for h in range(QH):
        qrot[h] = norm_rot(q_in[:, h * HD:(h + 1) * HD], qg_ref[...])

    def arrived(d):
        remote(block(d), block(d), w_z.at[0], w_recv.at[d], (sp, d)).wait_recv()

    def relay(i):
        d = z_peers[i] * n_x + x
        arrived(d)
        for k, xp in enumerate(x_peers):
            send(block(d), block(d), w_x.at[i + 1, k], w_recv.at[d], (sp, z * n_x + xp))

    relays = [functools.partial(relay, i) for i in range(n_z - 1)]
    for i, yp in enumerate(y_peers):
        j = yp * 2 + c
        remote(at(kbuf, j), at(kbuf, j), k_send.at[0], k_recv.at[yp], (j, dp)).wait_recv()
        send(at(kbuf, j), at(kbuf, j), k_fwd.at[i], k_frecv.at[yp], (sib, dp))
    for step_on in relays[:1]:
        step_on()
    for yp in [y] + y_peers:
        j = yp * 2 + 1 - c
        remote(at(kbuf, j), at(kbuf, j), k_send.at[0], k_frecv.at[yp], (sib, dp)).wait_recv()

    scale = HD ** -0.5 * math.log2(math.e)

    def weights(h, g):
        s = lax.dot_general(
            qrot[h], kbuf[:, g * HD:(g + 1) * HD], (((1,), (1,)), ((), ())),
            preferred_element_type=jnp.float32,
        )
        e = jnp.exp2((s - jnp.max(s, axis=-1, keepdims=True)) * scale)
        prob[h] = (e * (1.0 / jnp.sum(e, axis=-1, keepdims=True))).astype(jnp.bfloat16)

    relays = relays[1:]
    done = 0
    for part in range(GROUP // 2):
        count = len(relays) * part // (GROUP // 2 - 1) if part != 1 else -(-len(relays) // 2)
        for step_on in relays[done:count]:
            step_on()
        done = count
        for g in range(KVH):
            base = g * GROUP + part * 2

            @pl.loop(base, base + 2)
            def _(h, g=g):
                weights(h, g)

    for zz in [z] + z_peers:
        for xp in x_peers:
            arrived(zz * n_x + xp)
    theirs = token_part(1 - c)
    remote(theirs, theirs, t_send.at[0], t_recv.at[0], (sib, dp)).wait_recv()

    def chip(head, yy):
        return vbuf.at[head, pl.ds(pl.multiple_of(yy * 2 * rows, 16), 2 * rows), :]

    chip(c, y)[...] = jnp.dot(tok[...], wbuf[...], preferred_element_type=jnp.float32).astype(jnp.bfloat16)
    for i, yp in enumerate(y_peers):
        send(chip(c, y), chip(c, y), v_send.at[i], v_recv.at[y], (yp * 2 + c, dp))
    send(chip(c, y), chip(c, y), v_send.at[n_y - 1], v_frecv.at[y], (sib, dp))
    for i, yp in enumerate(y_peers):
        there = chip(c, yp)
        remote(there, there, v_send.at[0], v_recv.at[yp], (yp * 2 + c, dp)).wait_recv()
        send(there, there, v_fwd.at[i], v_frecv.at[yp], (sib, dp))

    def attend(core):
        for i in range(GROUP):
            h = core * GROUP + i
            out_ref[:, pl.ds(pl.multiple_of(h * HD, HD), HD)] = jnp.dot(
                prob[h], vbuf[core], preferred_element_type=jnp.float32
            ).astype(jnp.bfloat16)

    attend(c)
    for yp in [y] + y_peers:
        there = chip(1 - c, yp)
        remote(there, there, v_send.at[0], v_frecv.at[yp], (sib, dp)).wait_recv()
    attend(1 - c)
    for copy in pending:
        copy.wait_send()


def per_device(queries, keys, tokens, w_value, q_gain, k_gain):
    n_sp, n_dp = lax.axis_size("sp"), lax.axis_size("dp")
    n_x = inner_size(n_dp)
    n_z = n_dp // n_x
    n_y = n_sp // 2
    rows, width = tokens.shape[1:]
    depth = w_value.shape[0]
    any_spec = pl.BlockSpec(memory_space=pltpu.HBM)
    bf16, f32 = jnp.bfloat16, jnp.float32
    dma = pltpu.SemaphoreType.DMA
    length = rows * n_sp
    buffers = [
        ((rows, QH * HD), bf16),
        ((rows, KVH * HD), bf16),
        ((2 * rows, width), bf16),
        ((width, HD), bf16),
        ((length, KVH * HD), bf16),
        ((KVH, length, HD), bf16),
        ((QH, rows, HD), bf16),
        ((QH, rows, length), bf16),
        ((rows, HD), f32),
        ((rows, HD), f32),
        ((1, HD), f32),
        ((1, HD), f32),
    ]
    held = sum(math.prod(shape) * jnp.dtype(kind).itemsize for shape, kind in buffers)
    limit = min(60 * 2 ** 20, held + held // 4 + 8 * rows * length * 4 + 4 * 2 ** 20)
    operands = (queries[0], keys[0], tokens[0], w_value, q_gain[None], k_gain[None])
    operands = [pltpu.with_memory_space_constraint(a, pltpu.HBM) for a in operands]
    out = pl.pallas_call(
        functools.partial(kernel, n_sp, n_dp),
        out_shape=jax.ShapeDtypeStruct((rows, QH * HD), bf16),
        in_specs=[any_spec] * 6,
        out_specs=pl.BlockSpec(memory_space=pltpu.VMEM),
        scratch_shapes=[pltpu.VMEM(shape, kind) for shape, kind in buffers]
        + [
            dma((6,)),
            dma((n_z,)),
            dma((n_z, n_x)),
            dma((n_dp,)),
            dma((1,)),
            dma((1,)),
            dma((n_y,)),
            dma((n_y,)),
            dma((n_y,)),
            dma((n_y,)),
            dma((n_y,)),
            dma((n_y,)),
            dma((n_y,)),
            dma((n_y,)),
        ],
        compiler_params=pltpu.CompilerParams(
            collective_id=0, has_side_effects=True, vmem_limit_bytes=limit
        ),
        name="fused_attention",
    )(*operands)
    return out[None]


def solution(mesh):
    in_specs = (
        P("dp", "sp", None),
        P("dp", "sp", None),
        P("dp", "sp", None),
        P("dp", None),
        P(),
        P(),
    )
    return jax.shard_map(
        per_device, mesh=mesh, in_specs=in_specs, out_specs=P("dp", "sp", None), check_vma=False
    )
```
